768 devices in a mesh: sp: 96 (over z, y), tp: 8 (over x, core).
Axes of the slice: x: 4, y: 8, z: 12, core: 2. Of those that a mesh axis runs over, the one named last changes fastest.
Arguments:
- tokens: bfloat16 [18432, 2048], P(('sp', 'tp')), may hold values from -6 to 6
- norm_in: float32 [2048], replicated, may hold values from 0.1 to 1.9
- decay_log: float32 [128, 64], P('tp'), may hold values from -0.034 to -1.3563368e-05, as said below
- phase: float32 [128, 64], P('tp'), may hold values from -1 to 1
- b_real: float32 [128, 64, 16], P('tp'), may hold values from -1 to 1
- b_imag: float32 [128, 64, 16], P('tp'), may hold values from -1 to 1
- c_real: float32 [128, 16, 64], P('tp'), may hold values from -0.75 to 0.75
- c_imag: float32 [128, 16, 64], P('tp'), may hold values from -0.75 to 0.75
- skip_gain: float32 [2048], P('tp'), may hold values from -6 to 6
- w_value: bfloat16 [2048, 2048], P(None, 'tp'), as said below
- w_gate: bfloat16 [2048, 2048], P(None, 'tp'), may hold values from -0.125 to 0.125
- norm_out: float32 [2048], P('tp'), may hold values from 0.1 to 1.9
Outputs:
- mixed: bfloat16 [18432, 2048], P('sp', 'tp')
The draws below stay inside these ranges and needn't reach their ends.
Inputs may be any that keep to these rules, and one draw needn't show every extreme that they name: `decay_log`: negative real parts of the eigenvalues. `w_value`: weights of the value projection.
All inputs are finite; a program needn't handle non-finite values.
Results may differ from the reference program's by a relative error of at most 0.012.
The reference program's roundings to bfloat16 on the way count: a program that leaves them out, or rounds other values in their place, can miss the bound.
Values may be sent and summed in bfloat16 or wider, within the bound.
A program may use at most 32 MiB of HBM per device.

```python
import math
import jax
import jax.numpy as jnp
from jax import lax

D = 2048
GROUP = 16
STATE = 64
GROUPS = 128
TOK_DEV = 192
TOKENS = 18432
N_SP = 96


def draw_decay_log(key, part):
    first_key = jax.random.fold_in(key, 11)
    second_key = jax.random.fold_in(key, 12)
    third_key = jax.random.fold_in(key, 13)
    slow_share = 0.5
    slow_flag = jax.random.uniform(first_key, (GROUPS, 1), jnp.float32) < slow_share
    slow_rate = jnp.exp(jax.random.uniform(second_key, (GROUPS, STATE), jnp.float32, math.log(0.25), math.log(2.2))) / TOKENS
    fast_rate = jnp.exp(jax.random.uniform(third_key, (GROUPS, STATE), jnp.float32, math.log(0.0101), math.log(0.0333)))
    return -jnp.where(slow_flag, slow_rate, fast_rate)


def draw_w_value(key, part):
    top_scale = 10.0
    columns = jnp.arange(D, dtype=jnp.float32)
    column_scale = jnp.exp(math.log(top_scale) * columns / D)
    base = jax.random.normal(key, (D, D), jnp.float32) * D ** (-0.5)
    return (base * column_scale[None, :]).astype(jnp.bfloat16)


def block_levels(key, dims, shards, low, top_value):
    def one(dim, shards_of):
        steps = jax.random.uniform(jax.random.fold_in(jax.random.fold_in(key, 6), dim), (shards_of,), jnp.float32, low / len(shards), top_value / len(shards))
        return jnp.repeat(jnp.exp(steps), dims[dim] // shards_of).reshape((-1,) + (1,) * (len(dims) - dim - 1))

    level = one(*shards[0])
    for cut in shards[1:]:
        level = level * one(*cut)
    return level


def centred(rng, dims, spread, bound, cuts=(), kind=jnp.bfloat16):
    result = jax.random.normal(rng, dims, jnp.float32) * spread
    if len(cuts) > 0:
        result = block_levels(rng, dims, cuts, -0.22, 0.18) * result
    return jnp.clip(result, min=-bound, max=bound).astype(kind)


def setup_inputs(seed: int = 0) -> dict:
    splits = jax.random.split(jax.random.key(seed), 13)
    return {
        "tokens": centred(splits[0], (TOKENS, D), 1.0, 6.0, ((0, 768),)),
        "norm_in": jnp.clip(1.0 + 0.18 * jax.random.normal(splits[1], (D,), jnp.float32), 0.1, 1.9),
        "decay_log": draw_decay_log(jax.random.fold_in(splits[12], 71), 0),
        "phase": jnp.clip(jax.random.uniform(splits[3], (GROUPS, STATE), jnp.float32, -1.0, 1.0) * block_levels(splits[3], (GROUPS, STATE), ((0, 8),), -0.4, 0.0), -1.0, 1.0),
        "b_real": centred(splits[4], (GROUPS, STATE, GROUP), (2 * GROUP) ** -0.5, 1.0, ((0, 8),), jnp.float32),
        "b_imag": centred(splits[5], (GROUPS, STATE, GROUP), (2 * GROUP) ** -0.5, 1.0, ((0, 8),), jnp.float32),
        "c_real": centred(splits[6], (GROUPS, GROUP, STATE), STATE ** -0.5, 0.75, ((0, 8),), jnp.float32),
        "c_imag": centred(splits[7], (GROUPS, GROUP, STATE), STATE ** -0.5, 0.75, ((0, 8),), jnp.float32),
        "skip_gain": centred(splits[8], (D,), 1.0, 6.0, ((0, 8),), jnp.float32),
        "w_value": draw_w_value(jax.random.fold_in(splits[12], 71), 0),
        "w_gate": centred(splits[10], (D, D), D ** -0.5, 0.125, ((1, 8),)),
        "norm_out": jnp.clip(1.0 + 0.18 * jax.random.normal(splits[11], (D,), jnp.float32), 0.1, 1.9),
    }


NORM_EPS = 1e-06
HIGHEST_PREC = lax.Precision.HIGHEST

def coefficients(decay_log, phase, b_real, b_imag):
    magnitude = jnp.exp(decay_log)
    bar_re = magnitude * jnp.cos(phase)
    bar_im = magnitude * jnp.sin(phase)
    modulus = decay_log * decay_log + phase * phase
    coef_re = ((bar_re - 1.0) * decay_log + bar_im * phase) / modulus
    coef_im = (bar_im * decay_log - (bar_re - 1.0) * phase) / modulus
    in_re = coef_re[:, :, None] * b_real - coef_im[:, :, None] * b_imag
    in_im = coef_re[:, :, None] * b_imag + coef_im[:, :, None] * b_real
    return (bar_re, bar_im, in_re, in_im)

def prefix_states(drive_re, drive_im, rate_re, rate_im):
    length = drive_re.shape[0]
    stride = 1
    for level in range(max(length - 1, 1).bit_length()):
        padding = jnp.zeros((stride,) + drive_re.shape[1:], jnp.float32)
        moved_re = jnp.concatenate([padding, drive_re[:length - stride]], axis=0)
        moved_im = jnp.concatenate([padding, drive_im[:length - stride]], axis=0)
        drive_re, drive_im = (drive_re + rate_re * moved_re - rate_im * moved_im, drive_im + rate_re * moved_im + rate_im * moved_re)
        rate_re, rate_im = (rate_re * rate_re - rate_im * rate_im, 2.0 * rate_re * rate_im)
        stride = stride * 2
    return (drive_re, drive_im)

def readout(state_re, state_im, c_real, c_imag):
    first = jnp.einsum('tgp,ghp->tgh', state_re, c_real, precision=HIGHEST_PREC)
    second = jnp.einsum('tgp,ghp->tgh', state_im, c_imag, precision=HIGHEST_PREC)
    return first - second

def reference(tokens, norm_in, decay_log, phase, b_real, b_imag, c_real, c_imag, skip_gain, w_value, w_gate, norm_out):
    xf = tokens.astype(jnp.float32)
    normed = (xf * lax.rsqrt(lax.optimization_barrier(jnp.mean(xf * xf, axis=1, keepdims=True)) + NORM_EPS) * norm_in).astype(jnp.bfloat16)
    bar_re, bar_im, bb_re, bb_im = coefficients(decay_log, phase, b_real, b_imag)
    blocks = normed.reshape(N_SP, TOK_DEV, GROUPS, GROUP)
    skip_grid = skip_gain.reshape(GROUPS, GROUP)

    def block_step(carried, block):
        state_re, state_im = carried
        drive = block.astype(jnp.float32)
        in_re = jnp.einsum('tgh,gph->tgp', drive, bb_re, precision=HIGHEST_PREC)
        in_im = jnp.einsum('tgh,gph->tgp', drive, bb_im, precision=HIGHEST_PREC)
        in_re = in_re.at[0].add(bar_re * state_re - bar_im * state_im)
        in_im = in_im.at[0].add(bar_re * state_im + bar_im * state_re)
        all_re, all_im = prefix_states(in_re, in_im, bar_re, bar_im)
        mixed_pre = readout(all_re, all_im, c_real, c_imag) + skip_grid * drive
        z_block = jax.nn.gelu(mixed_pre).reshape(TOK_DEV, D).astype(jnp.bfloat16)
        return ((all_re[-1], all_im[-1]), z_block)
    start_state = (jnp.zeros((GROUPS, STATE), jnp.float32), jnp.zeros((GROUPS, STATE), jnp.float32))
    ignored, z_blocks = lax.scan(block_step, start_state, blocks)
    z_all = z_blocks.reshape(N_SP * TOK_DEV, D)
    projected_value = jnp.dot(z_all, w_value, preferred_element_type=jnp.float32)
    projected_gate = jnp.dot(z_all, w_gate, preferred_element_type=jnp.float32)
    gated = projected_value * jax.nn.sigmoid(projected_gate)
    scale = lax.rsqrt(lax.optimization_barrier(jnp.mean(gated * gated, axis=1, keepdims=True)) + NORM_EPS)
    return (gated * scale * norm_out).astype(jnp.bfloat16)
```

```python
import functools

import jax
import jax.numpy as jnp
from jax import lax
from jax.experimental import pallas as pl
from jax.experimental.pallas import tpu as pltpu
from jax.sharding import Mesh
from jax.sharding import PartitionSpec as P

D = 2048
SP = ("sp_0", "sp_1")
SP_TP = ("sp_0", "sp_1", "tp")
NORM_EPS = 1e-06

F32 = jnp.float32
BF16 = jnp.bfloat16
ROWS = 192
TP = 8
STEPS = 24
WIDTH = 256
GROUPS = 16
STATE = 64
PAIRS = 8
LANES = 128
MESH = pl.DeviceIdType.MESH


def cmul(a, b):
    return (a[0] * b[0] - a[1] * b[1], a[0] * b[1] + a[1] * b[0])


def cmuladd(a, b, c):
    return (a[0] * b[0] - a[1] * b[1] + c[0], a[0] * b[1] + a[1] * b[0] + c[1])


def split_store(dst, g, real, imag):
    pair, second = g // 2, g % 2
    blank = jnp.zeros((16, STATE), F32)
    wide = [jnp.concatenate([blank, part] if second else [part, blank], axis=1) for part in (real, imag)]
    full = jnp.concatenate(wide, axis=1)
    high = full.astype(BF16)
    low = (full - high.astype(F32)).astype(BF16)
    row = 32 * (pair % 4) + 16 * second
    dst[pair, row : row + 16, :] = high
    dst[pair, LANES + row : LANES + row + 16, :] = low


def kernel(
    nz,
    ny,
    tok,
    nin,
    dl,
    ph,
    b_re,
    b_im,
    c_re,
    c_im,
    skip,
    wv,
    wg,
    nout,
    out,
    tok_v,
    nin_v,
    dl_v,
    ph_v,
    b_v,
    c_v,
    skip_v,
    wv_v,
    wg_v,
    nout_v,
    xs,
    xr,
    uf,
    wb,
    ct,
    dbuf,
    coef_v,
    wide_v,
    lam_v,
    pow_v,
    hop_v,
    fbuf,
    es,
    yr,
    zs,
    zr,
    held_v,
    sbuf,
    yv,
    zg,
    acc,
    gbuf,
    ss,
    sr,
    of,
    in_sem,
    xs_sem,
    xr_sem,
    ys_sem,
    yr_sem,
    zs_sem,
    zr_sem,
    gs_sem,
    gr_sem,
    qs_sem,
    qr_sem,
):
    me_z, me_y, me = lax.axis_index("sp_0"), lax.axis_index("sp_1"), lax.axis_index("tp")

    loads = []
    for k, (src, dst) in enumerate(
        (
            (tok, tok_v),
            (nin, nin_v),
            (dl, dl_v),
            (ph, ph_v),
            (b_re, b_v.at[0]),
            (b_im, b_v.at[1]),
            (c_re, c_v.at[0]),
            (c_im, c_v.at[1]),
            (skip, skip_v),
            (nout, nout_v),
            (wv, wv_v),
            (wg, wg_v),
        )
    ):
        load = pltpu.make_async_copy(src, dst, in_sem.at[k])
        load.start()
        loads.append(load)

    barrier = pltpu.get_barrier_semaphore()
    for k in range(1, nz):
        pl.semaphore_signal(barrier, inc=1, device_id={"sp_0": lax.rem(me_z + k, nz)}, device_id_type=MESH)
    for k in range(1, ny):
        pl.semaphore_signal(barrier, inc=1, device_id={"sp_1": lax.rem(me_y + k, ny)}, device_id_type=MESH)
    for k in range(1, TP):
        pl.semaphore_signal(barrier, inc=1, device_id={"tp": lax.rem(me + k, TP)}, device_id_type=MESH)

    loads[0].wait()
    loads[1].wait()
    x = tok_v[...].astype(F32)
    mean = jnp.sum(x * x, axis=1, keepdims=True) * (1.0 / D)
    normed = (x * lax.rsqrt(mean + NORM_EPS) * nin_v[...]).astype(BF16)
    for k in range(TP):
        xs[k] = normed[:, k * WIDTH : (k + 1) * WIDTH]

    loads[2].wait()
    loads[3].wait()
    decay, phase = dl_v[...], ph_v[...]
    magnitude = jnp.exp(decay)
    bar_re, bar_im = magnitude * jnp.cos(phase), magnitude * jnp.sin(phase)
    modulus = decay * decay + phase * phase
    coef_v[0] = ((bar_re - 1.0) * decay + bar_im * phase) / modulus
    coef_v[1] = (bar_im * decay - (bar_re - 1.0) * phase) / modulus
    wide_v[0] = jnp.concatenate([bar_re, bar_re], axis=1)
    wide_v[1] = jnp.concatenate([bar_im, bar_im], axis=1)
    left_half = lax.broadcasted_iota(jnp.int32, (PAIRS, LANES), 1) < STATE
    lam = tuple(
        jnp.where(left_half, wide_v[k, pl.ds(0, PAIRS, stride=2), :], wide_v[k, pl.ds(1, PAIRS, stride=2), :])
        for k in range(2)
    )
    lam2 = cmul(lam, lam)
    lam4 = cmul(lam2, lam2)
    lam8 = cmul(lam4, lam4)
    seg = cmul(cmul(lam8, lam8), lam8)
    lam_v[0], lam_v[1] = lam
    power = (jnp.ones((PAIRS, LANES), F32), jnp.zeros((PAIRS, LANES), F32))
    for j in range(TP):
        pow_v[0, j * PAIRS : (j + 1) * PAIRS, :], pow_v[1, j * PAIRS : (j + 1) * PAIRS, :] = power
        power = cmul(power, seg)
    hop = power
    power = (jnp.ones((PAIRS, LANES), F32), jnp.zeros((PAIRS, LANES), F32))
    for y in range(ny):
        hop_v[y, 0], hop_v[y, 1] = power
        power = cmul(power, hop)
    line = power
    loads[4].wait()
    loads[5].wait()
    wb[...] = jnp.zeros_like(wb)
    for g in range(GROUPS):
        split_store(wb, g, b_v[0, 16 * g : 16 * g + 16, :], b_v[1, 16 * g : 16 * g + 16, :])

    pl.semaphore_wait(barrier, nz + ny + TP - 3)

    xcopies = []
    for k in range(1, TP):
        peer = lax.rem(me + k, TP)
        copy = pltpu.make_async_remote_copy(
            xs.at[peer], xr.at[me], xs_sem.at[k - 1], xr_sem.at[k - 1], device_id={"tp": peer}, device_id_type=MESH
        )
        copy.start()
        xcopies.append(copy)
    xr[me] = xs[me]
    for k in range(1, TP):
        source = lax.rem(me + TP - k, TP)
        pltpu.make_async_remote_copy(
            xs.at[source], xr.at[source], xs_sem.at[k - 1], xr_sem.at[k - 1], device_id={"tp": source}, device_id_type=MESH
        ).wait_recv()

    for j in range(TP):
        block = xr[j].astype(F32)
        for q in range(2):
            uf[q, j * STEPS : (j + 1) * STEPS, :] = block[:, q * LANES : (q + 1) * LANES]
    for q in range(2):
        half = uf[q].astype(BF16)
        twice = jnp.concatenate([half, half], axis=1)
        for pair in range(4 * q, 4 * q + 4):
            drive = jnp.dot(twice, wb[pair], preferred_element_type=F32)
            dbuf[pair, 0] = drive[:, :LANES]
            dbuf[pair, 1] = drive[:, LANES:]

    def rate(pair):
        return tuple(jnp.broadcast_to(lam_v[k, pair : pair + 1, :], (TP, LANES)) for k in range(2))

    rates = [rate(pair) for pair in range(PAIRS)]

    def drive_at(pair, i):
        return (dbuf[pair, 0, pl.ds(i, TP, stride=STEPS), :], dbuf[pair, 1, pl.ds(i, TP, stride=STEPS), :])

    def first_pass(i, states):
        states = list(states)
        for sub in range(2):
            for pair in range(PAIRS):
                states[pair] = cmuladd(rates[pair], states[pair], drive_at(pair, 2 * i + sub))
        return tuple(states)

    nothing = jnp.zeros((TP, LANES), F32)
    ends = lax.fori_loop(0, STEPS // 2, first_pass, tuple((nothing, nothing) for _ in range(PAIRS)))
    segment = lax.broadcasted_iota(jnp.int32, (TP, LANES), 0)
    for pair in range(PAIRS):
        total = ends[pair]
        for shift in (1, 2, 4):
            moved = tuple(jnp.where(segment >= shift, pltpu.roll(part, shift, 0), 0.0) for part in total)
            decay_of = tuple(
                jnp.broadcast_to(pow_v[k, shift * PAIRS + pair : shift * PAIRS + pair + 1, :], (TP, LANES))
                for k in range(2)
            )
            total = cmuladd(decay_of, moved, total)
        for k in range(2):
            es[k, pair : pair + 1, :] = total[k][TP - 1 : TP, :]
            fbuf[pair, k] = jnp.where(segment >= 1, pltpu.roll(total[k], 1, 0), 0.0)

    ycopies = []
    for k in range(1, ny):
        peer = lax.rem(me_y + k, ny)
        copy = pltpu.make_async_remote_copy(
            es, yr.at[me_y], ys_sem.at[k - 1], yr_sem.at[k - 1], device_id={"sp_1": peer}, device_id_type=MESH
        )
        copy.start()
        ycopies.append(copy)
    yr[me_y] = es[...]

    loads[6].wait()
    loads[7].wait()
    ct[...] = jnp.zeros_like(ct)
    for g in range(GROUPS):
        own = (c_v[0, 16 * g : 16 * g + 16, :], c_v[1, 16 * g : 16 * g + 16, :])
        real, imag = cmul(own, (coef_v[0, g : g + 1, :], coef_v[1, g : g + 1, :]))
        split_store(ct, g, real, -imag)

    for k in range(1, ny):
        source = lax.rem(me_y + ny - k, ny)
        pltpu.make_async_remote_copy(
            es, yr.at[source], ys_sem.at[k - 1], yr_sem.at[k - 1], device_id={"sp_1": source}, device_id_type=MESH
        ).wait_recv()
    empty = (jnp.zeros((PAIRS, LANES), F32), jnp.zeros((PAIRS, LANES), F32))
    total, inside = empty, empty
    for y in range(ny):
        inside = tuple(jnp.where(me_y == y, new, old) for new, old in zip(total, inside))
        total = cmuladd(hop, total, (yr[y, 0], yr[y, 1]))
    zs[0], zs[1] = total

    def zcopy(k, peer, slot):
        return pltpu.make_async_remote_copy(
            zs, zr.at[slot], zs_sem.at[k - 1], zr_sem.at[k - 1], device_id={"sp_0": peer}, device_id_type=MESH
        )

    for k in range(1, nz):

        @pl.when(me_z + k < nz)
        def _(k=k):
            zcopy(k, me_z + k, me_z).start()

    held_v[...] = jnp.zeros_like(held_v)
    for k in range(nz - 1, 0, -1):

        @pl.when(me_z >= k)
        def _(k=k):
            zcopy(k, me_z - k, me_z - k).wait_recv()
            new = cmuladd(line, (held_v[0], held_v[1]), (zr[me_z - k, 0], zr[me_z - k, 1]))
            held_v[0], held_v[1] = new

    held = cmuladd((hop_v[me_y, 0], hop_v[me_y, 1]), (held_v[0], held_v[1]), inside)
    held_v[0], held_v[1] = held

    starts = []
    for pair in range(PAIRS):
        carried = tuple(jnp.broadcast_to(held_v[k, pair : pair + 1, :], (TP, LANES)) for k in range(2))
        reach = tuple(pow_v[k, pl.ds(pair, TP, stride=PAIRS), :] for k in range(2))
        starts.append(cmuladd(reach, carried, (fbuf[pair, 0], fbuf[pair, 1])))

    def second_pass(i, states):
        states = list(states)
        row = pl.multiple_of(2 * TP * i, 2 * TP)
        for pair in range(PAIRS):
            one = cmuladd(rates[pair], states[pair], drive_at(pair, 2 * i))
            two = cmuladd(rates[pair], one, drive_at(pair, 2 * i + 1))
            for k in range(2):
                both = jnp.concatenate([one[k], two[k]], axis=0).astype(BF16)
                sbuf[pair, pl.ds(row, 2 * TP), k * LANES : (k + 1) * LANES] = both
            states[pair] = two
        return tuple(states)

    lax.fori_loop(0, STEPS // 2, second_pass, tuple(starts))

    loads[8].wait()
    for q in range(2):
        both = None
        for pair in range(4 * q, 4 * q + 4):
            part = lax.dot_general(sbuf[pair], ct[pair], (((1,), (1,)), ((), ())), preferred_element_type=F32)
            both = part if both is None else both + part
        yv[q] = both[:, :LANES] + both[:, LANES:]

    def activate(i, _):
        row = pl.multiple_of(2 * TP * i, 2 * TP)
        for q in range(2):
            gain = skip_v[:, q * LANES : (q + 1) * LANES]
            direct = jnp.concatenate([uf[q, pl.ds(2 * i + sub, TP, stride=STEPS), :] for sub in range(2)], axis=0)
            pre = yv[q, pl.ds(row, 2 * TP), :] + gain * direct
            z = jax.nn.gelu(pre)
            zg[me, pl.ds(row, 2 * TP), q * LANES : (q + 1) * LANES] = z.astype(BF16)
        return 0

    lax.fori_loop(0, STEPS // 2, activate, 0)

    chip, core = lax.div(me, 2), lax.rem(me, 2)
    partner = me + 1 - 2 * core
    right = lax.rem(chip + 1, TP // 2) * 2 + core
    left = lax.rem(chip + TP // 2 - 1, TP // 2) * 2 + core
    far = lax.rem(chip + 2, TP // 2) * 2 + core
    other = 1 - 2 * core

    def gcopy(n, owner, half, peer):
        part = zg.at[owner, pl.ds(half * (ROWS // 2), ROWS // 2), :]
        return pltpu.make_async_remote_copy(
            part, part, gs_sem.at[n], gr_sem.at[n], device_id={"tp": peer}, device_id_type=MESH
        )

    def send(n, owner, half, peer):
        gcopy(n, owner, half, peer).start()

    def arrived(n, owner, half, peer):
        gcopy(n, owner, half, peer).wait_recv()

    for half in range(2):
        send(half, me, half, right)
        send(2 + half, me, half, left)
        send(4 + half, me, half, partner)

    def project(owner, first=False):
        rows = pl.ds(pl.multiple_of(owner * WIDTH, WIDTH), WIDTH)
        block = zg[owner]
        for k, weight in enumerate((wv_v, wg_v)):
            part = jnp.dot(block, weight[rows, :], preferred_element_type=F32)
            if first:
                acc[k] = part
            else:
                acc[k] += part

    loads[10].wait()
    loads[11].wait()
    project(me, first=True)
    arrived(0, left, 0, left)
    send(6, left, 0, right)
    send(8, left, 0, partner)
    arrived(2, right, 0, right)
    send(10, right, 0, partner)
    arrived(4, partner, 0, partner)
    arrived(5, partner, 1, partner)
    project(partner)
    arrived(3, right, 1, right)
    send(7, right, 1, left)
    send(11, right, 1, partner)
    arrived(1, left, 1, left)
    send(9, left, 1, partner)
    project(right)
    project(left)
    arrived(6, far, 0, left)
    send(12, far, 0, partner)
    arrived(7, far, 1, right)
    send(13, far, 1, partner)
    for half in range(2):
        arrived(8 + half, left + other, half, partner)
    project(left + other)
    for half in range(2):
        arrived(10 + half, right + other, half, partner)
    project(right + other)
    project(far)
    for half in range(2):
        arrived(12 + half, far + other, half, partner)
    project(far + other)

    ss[...] = jnp.zeros_like(ss)
    lane = lax.broadcasted_iota(jnp.int32, (TP, LANES), 1)

    def gate(i, _):
        rows = pl.ds(pl.multiple_of(TP * i, TP), TP)
        gated = acc[0, rows, :] * jax.nn.sigmoid(acc[1, rows, :])
        gbuf[rows, :] = gated
        own = jnp.sum(gated * gated, axis=1, keepdims=True)
        ss[...] = jnp.where(lane == i, own, ss[...])
        return 0

    lax.fori_loop(0, STEPS, gate, 0)
    qcopies = []
    for k in range(1, TP):
        peer = lax.rem(me + k, TP)
        copy = pltpu.make_async_remote_copy(
            ss, sr.at[me], qs_sem.at[k - 1], qr_sem.at[k - 1], device_id={"tp": peer}, device_id_type=MESH
        )
        copy.start()
        qcopies.append(copy)
    sr[me] = ss[...]
    loads[9].wait()
    for k in range(1, TP):
        source = lax.rem(me + TP - k, TP)
        pltpu.make_async_remote_copy(
            ss, sr.at[source], qs_sem.at[k - 1], qr_sem.at[k - 1], device_id={"tp": source}, device_id_type=MESH
        ).wait_recv()
    squares = sr[0]
    for k in range(1, TP):
        squares = squares + sr[k]
    scale = lax.rsqrt(squares * (1.0 / D) + NORM_EPS)
    for i in range(STEPS):
        done = gbuf[i * TP : (i + 1) * TP, :] * scale[:, i : i + 1] * nout_v[...]
        for q in range(2):
            of[q, pl.ds(i, TP, stride=STEPS), :] = done[:, q * LANES : (q + 1) * LANES]
    for q in range(2):
        out[:, q * LANES : (q + 1) * LANES] = of[q].astype(BF16)

    for copy in xcopies + ycopies + qcopies:
        copy.wait_send()
    for k in range(1, nz):

        @pl.when(me_z + k < nz)
        def _(k=k):
            zcopy(k, me_z + k, me_z).wait_send()

    for n in range(14):
        gcopy(n, me, 0, partner).wait_send()


def on_device(nz, ny, tokens, norm_in, decay_log, phase, b_real, b_imag, c_real, c_imag, skip_gain, w_value, w_gate, norm_out):
    def by_channel(b):
        return b.transpose(0, 2, 1).reshape(WIDTH, STATE)

    dma = pltpu.SemaphoreType.DMA
    scratch = [
        pltpu.VMEM((STEPS, D), BF16),
        pltpu.VMEM((1, D), F32),
        pltpu.VMEM((GROUPS, STATE), F32),
        pltpu.VMEM((GROUPS, STATE), F32),
        pltpu.VMEM((2, WIDTH, STATE), F32),
        pltpu.VMEM((2, WIDTH, STATE), F32),
        pltpu.VMEM((1, WIDTH), F32),
        pltpu.VMEM((D, WIDTH), BF16),
        pltpu.VMEM((D, WIDTH), BF16),
        pltpu.VMEM((1, WIDTH), F32),
        pltpu.VMEM((TP, STEPS, WIDTH), BF16),
        pltpu.VMEM((TP, STEPS, WIDTH), BF16),
        pltpu.VMEM((2, ROWS, LANES), F32),
        pltpu.VMEM((PAIRS, 2 * LANES, 2 * LANES), BF16),
        pltpu.VMEM((PAIRS, 2 * LANES, 2 * LANES), BF16),
        pltpu.VMEM((PAIRS, 2, ROWS, LANES), F32),
        pltpu.VMEM((2, GROUPS, STATE), F32),
        pltpu.VMEM((2, GROUPS, LANES), F32),
        pltpu.VMEM((2, PAIRS, LANES), F32),
        pltpu.VMEM((2, TP * PAIRS, LANES), F32),
        pltpu.VMEM((ny, 2, PAIRS, LANES), F32),
        pltpu.VMEM((PAIRS, 2, TP, LANES), F32),
        pltpu.VMEM((2, PAIRS, LANES), F32),
        pltpu.VMEM((ny, 2, PAIRS, LANES), F32),
        pltpu.VMEM((2, PAIRS, LANES), F32),
        pltpu.VMEM((nz, 2, PAIRS, LANES), F32),
        pltpu.VMEM((2, PAIRS, LANES), F32),
        pltpu.VMEM((PAIRS, ROWS, 2 * LANES), BF16),
        pltpu.VMEM((2, ROWS, LANES), F32),
        pltpu.VMEM((TP, ROWS, WIDTH), BF16),
        pltpu.VMEM((2, ROWS, WIDTH), F32),
        pltpu.VMEM((ROWS, WIDTH), F32),
        pltpu.VMEM((TP, LANES), F32),
        pltpu.VMEM((TP, TP, LANES), F32),
        pltpu.VMEM((2, ROWS, LANES), F32),
        dma((12,)),
        dma((TP - 1,)),
        dma((TP - 1,)),
        dma((ny - 1,)),
        dma((ny - 1,)),
        dma((nz - 1,)),
        dma((nz - 1,)),
        dma((14,)),
        dma((14,)),
        dma((TP - 1,)),
        dma((TP - 1,)),
    ]
    return pl.pallas_call(
        functools.partial(kernel, nz, ny),
        out_shape=jax.ShapeDtypeStruct((ROWS, WIDTH), BF16),
        in_specs=[pl.BlockSpec(memory_space=pl.ANY)] * 12,
        out_specs=pl.BlockSpec(memory_space=pltpu.VMEM),
        scratch_shapes=scratch,
        compiler_params=pltpu.CompilerParams(
            collective_id=0, has_side_effects=True, vmem_limit_bytes=48 * 1024 * 1024
        ),
        name="mixer",
    )(
        tokens,
        norm_in.reshape(1, D),
        decay_log,
        phase,
        by_channel(b_real),
        by_channel(b_imag),
        c_real.reshape(WIDTH, STATE),
        c_imag.reshape(WIDTH, STATE),
        skip_gain.reshape(1, WIDTH),
        w_value,
        w_gate,
        norm_out.reshape(1, WIDTH),
    )


def solution(mesh):
    torus = Mesh(mesh.devices.reshape(-1, 8, mesh.shape["tp"]), SP_TP)
    return on_torus(torus)


def on_torus(torus):
    in_specs = (
        P(SP_TP, None),
        P(),
        P("tp", None),
        P("tp", None),
        P("tp", None, None),
        P("tp", None, None),
        P("tp", None, None),
        P("tp", None, None),
        P("tp"),
        P(None, "tp"),
        P(None, "tp"),
        P("tp"),
    )
    return jax.shard_map(
        functools.partial(on_device, torus.shape["sp_0"], torus.shape["sp_1"]),
        mesh=torus,
        in_specs=in_specs,
        out_specs=P(SP, "tp"),
        check_vma=False,
    )
```

```python
import functools

import jax
import jax.numpy as jnp
from jax import lax
from jax.experimental import pallas as pl
from jax.experimental.pallas import tpu as pltpu
from jax.sharding import Mesh
from jax.sharding import PartitionSpec as P

D = 2048
SP = ("sp_0", "sp_1")
SP_TP = ("sp_0", "sp_1", "tp")
NORM_EPS = 1e-06

F32 = jnp.float32
BF16 = jnp.bfloat16
ROWS = 192
TP = 8
STEPS = 24
WIDTH = 256
GROUPS = 16
STATE = 64
PAIRS = 8
LANES = 128
CHAIN = 4
FAR_FIRST = (4, 3, 5, 2, 6, 1, 7)
CHUNKS = 4
MESH = pl.DeviceIdType.MESH


def cmul(a, b):
    return (a[0] * b[0] - a[1] * b[1], a[0] * b[1] + a[1] * b[0])


def cmuladd(a, b, c):
    return (a[0] * b[0] - a[1] * b[1] + c[0], a[0] * b[1] + a[1] * b[0] + c[1])


def split_store(dst, g, real, imag):
    pair, second = g // 2, g % 2
    blank = jnp.zeros((16, STATE), F32)
    wide = [jnp.concatenate([blank, part] if second else [part, blank], axis=1) for part in (real, imag)]
    full = jnp.concatenate(wide, axis=1)
    high = full.astype(BF16)
    low = (full - high.astype(F32)).astype(BF16)
    row = 32 * (pair % 4) + 16 * second
    dst[pair, row : row + 16, :] = high
    dst[pair, LANES + row : LANES + row + 16, :] = low


def kernel(
    nz,
    ny,
    tok,
    nin,
    dl,
    ph,
    b_re,
    b_im,
    c_re,
    c_im,
    skip,
    wv,
    wg,
    nout,
    out,
    tok_v,
    nin_v,
    dl_v,
    ph_v,
    b_v,
    c_v,
    skip_v,
    wv_v,
    wg_v,
    nout_v,
    xs,
    xr,
    uf,
    wb,
    ct,
    dbuf,
    coef_v,
    wide_v,
    lam_v,
    pow_v,
    hop_v,
    fbuf,
    es,
    yr,
    zs,
    zr,
    held_v,
    sbuf,
    yv,
    zg,
    acc,
    gbuf,
    ss,
    sr,
    of,
    in_sem,
    xs_sem,
    xr_sem,
    ys_sem,
    yr_sem,
    zs_sem,
    zr_sem,
    here_sem,
    gs_sem,
    gr_sem,
    ps_sem,
    pr_sem,
    qs_sem,
    qr_sem,
):
    me_z, me_y, me = lax.axis_index("sp_0"), lax.axis_index("sp_1"), lax.axis_index("tp")
    y_order = [k for k in FAR_FIRST if k < ny]
    reach = min(CHAIN, nz - 1)

    loads = [
        pltpu.make_async_copy(src, dst, in_sem.at[k])
        for k, (src, dst) in enumerate(
            (
                (tok, tok_v),
                (nin, nin_v),
                (dl, dl_v),
                (ph, ph_v),
                (b_re, b_v.at[0]),
                (b_im, b_v.at[1]),
                (c_re, c_v.at[0]),
                (c_im, c_v.at[1]),
                (skip, skip_v),
                (nout, nout_v),
                (wv, wv_v),
                (wg, wg_v),
            )
        )
    ]
    for load in loads[:4]:
        load.start()

    barrier = pltpu.get_barrier_semaphore()
    for k in FAR_FIRST:
        pl.semaphore_signal(barrier, inc=1, device_id={"tp": lax.rem(me + k, TP)}, device_id_type=MESH)
    for k in y_order:
        pl.semaphore_signal(barrier, inc=1, device_id={"sp_1": lax.rem(me_y + k, ny)}, device_id_type=MESH)

    @pl.when(me_z > 0)
    def _():
        pl.semaphore_signal(barrier, inc=1, device_id={"sp_0": me_z - 1}, device_id_type=MESH)

    @pl.when(me_z + 1 < nz)
    def _():
        pl.semaphore_signal(barrier, inc=1, device_id={"sp_0": me_z + 1}, device_id_type=MESH)

    for load in loads[4:]:
        load.start()

    def tell(r):
        @pl.when((me_z > 0) & (me_z + r < nz))
        def _():
            pl.semaphore_signal(here_sem.at[r - 1], inc=1, device_id={"sp_0": me_z - 1}, device_id_type=MESH)

    def hear(r):
        @pl.when(me_z + 1 + r < nz)
        def _():
            pl.semaphore_wait(here_sem.at[r - 1], 1)

    loads[0].wait()
    loads[1].wait()
    x = tok_v[...].astype(F32)
    mean = jnp.sum(x * x, axis=1, keepdims=True) * (1.0 / D)
    normed = (x * lax.rsqrt(mean + NORM_EPS) * nin_v[...]).astype(BF16)
    for k in range(TP):
        xs[k] = normed[:, k * WIDTH : (k + 1) * WIDTH]

    loads[2].wait()
    loads[3].wait()
    decay, phase = dl_v[...], ph_v[...]
    magnitude = jnp.exp(decay)
    bar_re, bar_im = magnitude * jnp.cos(phase), magnitude * jnp.sin(phase)
    modulus = decay * decay + phase * phase
    coef_v[0] = ((bar_re - 1.0) * decay + bar_im * phase) / modulus
    coef_v[1] = (bar_im * decay - (bar_re - 1.0) * phase) / modulus
    wide_v[0] = jnp.concatenate([bar_re, bar_re], axis=1)
    wide_v[1] = jnp.concatenate([bar_im, bar_im], axis=1)
    left_half = lax.broadcasted_iota(jnp.int32, (PAIRS, LANES), 1) < STATE
    lam = tuple(
        jnp.where(left_half, wide_v[k, pl.ds(0, PAIRS, stride=2), :], wide_v[k, pl.ds(1, PAIRS, stride=2), :])
        for k in range(2)
    )
    lam2 = cmul(lam, lam)
    lam4 = cmul(lam2, lam2)
    lam8 = cmul(lam4, lam4)
    seg = cmul(cmul(lam8, lam8), lam8)
    lam_v[0], lam_v[1] = lam
    power = (jnp.ones((PAIRS, LANES), F32), jnp.zeros((PAIRS, LANES), F32))
    for j in range(TP):
        pow_v[0, j * PAIRS : (j + 1) * PAIRS, :], pow_v[1, j * PAIRS : (j + 1) * PAIRS, :] = power
        power = cmul(power, seg)
    hop = power
    power = (jnp.ones((PAIRS, LANES), F32), jnp.zeros((PAIRS, LANES), F32))
    for y in range(ny):
        hop_v[y, 0], hop_v[y, 1] = power
        power = cmul(power, hop)
    line = power
    loads[4].wait()
    loads[5].wait()
    wb[...] = jnp.zeros_like(wb)
    for g in range(GROUPS):
        split_store(wb, g, b_v[0, 16 * g : 16 * g + 16, :], b_v[1, 16 * g : 16 * g + 16, :])

    neighbours = jnp.minimum(me_z, 1) + jnp.minimum(nz - 1 - me_z, 1)
    pl.semaphore_wait(barrier, ny + TP - 2 + neighbours)
    tell(1)

    xcopies = []
    for k in FAR_FIRST:
        peer = lax.rem(me + k, TP)
        copy = pltpu.make_async_remote_copy(
            xs.at[peer], xr.at[me], xs_sem.at[k - 1], xr_sem.at[k - 1], device_id={"tp": peer}, device_id_type=MESH
        )
        copy.start()
        xcopies.append(copy)
    xr[me] = xs[me]
    for k in range(1, TP):
        source = lax.rem(me + TP - k, TP)
        pltpu.make_async_remote_copy(
            xs.at[source], xr.at[source], xs_sem.at[k - 1], xr_sem.at[k - 1], device_id={"tp": source}, device_id_type=MESH
        ).wait_recv()

    if reach > 1:
        hear(1)
        tell(2)

    for j in range(TP):
        block = xr[j].astype(F32)
        for q in range(2):
            uf[q, j * STEPS : (j + 1) * STEPS, :] = block[:, q * LANES : (q + 1) * LANES]
    for q in range(2):
        half = uf[q].astype(BF16)
        twice = jnp.concatenate([half, half], axis=1)
        for pair in range(4 * q, 4 * q + 4):
            drive = jnp.dot(twice, wb[pair], preferred_element_type=F32)
            dbuf[pair, 0] = drive[:, :LANES]
            dbuf[pair, 1] = drive[:, LANES:]

    def rate(pair):
        return tuple(jnp.broadcast_to(lam_v[k, pair : pair + 1, :], (TP, LANES)) for k in range(2))

    rates = [rate(pair) for pair in range(PAIRS)]

    def drive_at(pair, i):
        return (dbuf[pair, 0, pl.ds(i, TP, stride=STEPS), :], dbuf[pair, 1, pl.ds(i, TP, stride=STEPS), :])

    def first_pass(i, states):
        states = list(states)
        for sub in range(2):
            for pair in range(PAIRS):
                states[pair] = cmuladd(rates[pair], states[pair], drive_at(pair, 2 * i + sub))
        return tuple(states)

    nothing = jnp.zeros((TP, LANES), F32)
    ends = lax.fori_loop(0, STEPS // 2, first_pass, tuple((nothing, nothing) for _ in range(PAIRS)))
    segment = lax.broadcasted_iota(jnp.int32, (TP, LANES), 0)
    for pair in range(PAIRS):
        total = ends[pair]
        for shift in (1, 2, 4):
            moved = tuple(jnp.where(segment >= shift, pltpu.roll(part, shift, 0), 0.0) for part in total)
            decay_of = tuple(
                jnp.broadcast_to(pow_v[k, shift * PAIRS + pair : shift * PAIRS + pair + 1, :], (TP, LANES))
                for k in range(2)
            )
            total = cmuladd(decay_of, moved, total)
        for k in range(2):
            es[k, pair : pair + 1, :] = total[k][TP - 1 : TP, :]
            fbuf[pair, k] = jnp.where(segment >= 1, pltpu.roll(total[k], 1, 0), 0.0)

    ycopies = []
    for k in y_order:
        peer = lax.rem(me_y + k, ny)
        copy = pltpu.make_async_remote_copy(
            es, yr.at[me_y], ys_sem.at[k - 1], yr_sem.at[k - 1], device_id={"sp_1": peer}, device_id_type=MESH
        )
        copy.start()
        ycopies.append(copy)
    yr[me_y] = es[...]

    loads[6].wait()
    loads[7].wait()
    ct[...] = jnp.zeros_like(ct)
    for g in range(GROUPS):
        own = (c_v[0, 16 * g : 16 * g + 16, :], c_v[1, 16 * g : 16 * g + 16, :])
        real, imag = cmul(own, (coef_v[0, g : g + 1, :], coef_v[1, g : g + 1, :]))
        split_store(ct, g, real, -imag)

    for k in range(1, ny):
        source = lax.rem(me_y + ny - k, ny)
        pltpu.make_async_remote_copy(
            es, yr.at[source], ys_sem.at[k - 1], yr_sem.at[k - 1], device_id={"sp_1": source}, device_id_type=MESH
        ).wait_recv()
    empty = (jnp.zeros((PAIRS, LANES), F32), jnp.zeros((PAIRS, LANES), F32))
    total, inside = empty, empty
    for y in range(ny):
        inside = tuple(jnp.where(me_y == y, new, old) for new, old in zip(total, inside))
        total = cmuladd(hop, total, (yr[y, 0], yr[y, 1]))
    zs[0, 0], zs[0, 1] = total
    def zcopy(k, peer):
        return pltpu.make_async_remote_copy(
            zs.at[k // CHAIN],
            zr.at[k - 1],
            zs_sem.at[k - 1],
            zr_sem.at[k - 1],
            device_id={"sp_0": peer},
            device_id_type=MESH,
        )

    def zsend(k):
        @pl.when(me_z + k < nz)
        def _():
            zcopy(k, me_z + k).start()

    zsend(1)
    for k in range(2, min(reach, CHAIN - 1) + 1):
        if k > 2:
            hear(k - 1)
            tell(k)
        zsend(k)
    held_v[...] = jnp.zeros_like(held_v)
    for k in range(reach, 0, -1):

        @pl.when(me_z >= k)
        def _(k=k):
            zcopy(k, me_z - k).wait_recv()
            new = cmuladd(line, (held_v[0], held_v[1]), (zr[k - 1, 0], zr[k - 1, 1]))
            held_v[0], held_v[1] = new

    if reach == CHAIN:
        zs[1, 0], zs[1, 1] = cmuladd(line, (held_v[0], held_v[1]), total)
        hear(CHAIN - 1)
        zsend(CHAIN)
    held = cmuladd((hop_v[me_y, 0], hop_v[me_y, 1]), (held_v[0], held_v[1]), inside)
    held_v[0], held_v[1] = held

    starts = []
    for pair in range(PAIRS):
        carried = tuple(jnp.broadcast_to(held_v[k, pair : pair + 1, :], (TP, LANES)) for k in range(2))
        since = tuple(pow_v[k, pl.ds(pair, TP, stride=PAIRS), :] for k in range(2))
        starts.append(cmuladd(since, carried, (fbuf[pair, 0], fbuf[pair, 1])))

    def second_pass(i, states):
        states = list(states)
        row = pl.multiple_of(2 * TP * i, 2 * TP)
        for pair in range(PAIRS):
            one = cmuladd(rates[pair], states[pair], drive_at(pair, 2 * i))
            two = cmuladd(rates[pair], one, drive_at(pair, 2 * i + 1))
            for k in range(2):
                both = jnp.concatenate([one[k], two[k]], axis=0).astype(BF16)
                sbuf[pair, pl.ds(row, 2 * TP), k * LANES : (k + 1) * LANES] = both
            states[pair] = two
        return tuple(states)

    lax.fori_loop(0, STEPS // 2, second_pass, tuple(starts))

    loads[8].wait()
    for q in range(2):
        both = None
        for pair in range(4 * q, 4 * q + 4):
            part = lax.dot_general(sbuf[pair], ct[pair], (((1,), (1,)), ((), ())), preferred_element_type=F32)
            both = part if both is None else both + part
        yv[q] = both[:, :LANES] + both[:, LANES:]

    def activate(i, _):
        row = pl.multiple_of(2 * TP * i, 2 * TP)
        for q in range(2):
            gain = skip_v[:, q * LANES : (q + 1) * LANES]
            direct = jnp.concatenate([uf[q, pl.ds(2 * i + sub, TP, stride=STEPS), :] for sub in range(2)], axis=0)
            pre = yv[q, pl.ds(row, 2 * TP), :] + gain * direct
            z = jax.nn.gelu(pre)
            zg[me, pl.ds(row, 2 * TP), q * LANES : (q + 1) * LANES] = z.astype(BF16)
        return 0

    lax.fori_loop(0, STEPS // 2, activate, 0)

    chip, core = lax.div(me, 2), lax.rem(me, 2)
    partner = me + 1 - 2 * core
    right = lax.rem(chip + 1, TP // 2) * 2 + core
    left = lax.rem(chip + TP // 2 - 1, TP // 2) * 2 + core
    far = lax.rem(chip + 2, TP // 2) * 2 + core
    other = 1 - 2 * core

    def rows_of(owner, chunk, count):
        return zg.at[owner, pl.ds(chunk * (ROWS // CHUNKS), count * (ROWS // CHUNKS)), :]

    def gcopy(n, owner, chunk, peer):
        part = rows_of(owner, chunk, 1)
        return pltpu.make_async_remote_copy(
            part, part, gs_sem.at[n], gr_sem.at[n], device_id={"tp": peer}, device_id_type=MESH
        )

    def pcopy(n, owner, chunk, count):
        part = rows_of(owner, chunk, count)
        return pltpu.make_async_remote_copy(
            part, part, ps_sem.at[n], pr_sem.at[n], device_id={"tp": partner}, device_id_type=MESH
        )

    def project(owner, first=False):
        rows = pl.ds(pl.multiple_of(owner * WIDTH, WIDTH), WIDTH)
        block = zg[owner]
        for k, weight in enumerate((wv_v, wg_v)):
            part = jnp.dot(block, weight[rows, :], preferred_element_type=F32)
            if first:
                acc[k] = part
            else:
                acc[k] += part

    right_order, left_order = (0, 1, 2, 3), (2, 3, 0, 1)
    for k in range(CHUNKS):
        gcopy(right_order[k], me, right_order[k], right).start()
        gcopy(4 + left_order[k], me, left_order[k], left).start()
        if k == 0:
            pcopy(0, me, 0, CHUNKS).start()

    loads[10].wait()
    loads[11].wait()
    project(me, first=True)
    pcopy(0, partner, 0, CHUNKS).wait_recv()
    project(partner)
    for k in range(2):
        gcopy(k, left, k, left).wait_recv()
        gcopy(8 + k, left, k, right).start()
        gcopy(4 + 2 + k, right, 2 + k, right).wait_recv()
        gcopy(8 + 2 + k, right, 2 + k, left).start()
    pcopy(1, left, 0, 2).start()
    pcopy(2, right, 2, 2).start()
    for k in range(2):
        gcopy(2 + k, left, 2 + k, left).wait_recv()
        gcopy(4 + k, right, k, right).wait_recv()
    pcopy(3, left, 2, 2).start()
    pcopy(4, right, 0, 2).start()
    project(left)
    project(right)
    for k in range(2):
        gcopy(8 + k, far, k, left).wait_recv()
        gcopy(12 + k, far, k, partner).start()
        gcopy(8 + 2 + k, far, 2 + k, right).wait_recv()
        gcopy(12 + 2 + k, far, 2 + k, partner).start()
    pcopy(1, left + other, 0, 2).wait_recv()
    pcopy(3, left + other, 2, 2).wait_recv()
    project(left + other)
    pcopy(2, right + other, 2, 2).wait_recv()
    pcopy(4, right + other, 0, 2).wait_recv()
    project(right + other)
    project(far)
    for k in range(CHUNKS):
        gcopy(12 + k, far + other, k, partner).wait_recv()
    project(far + other)

    lane = lax.broadcasted_iota(jnp.int32, (TP, LANES), 1)
    sums = jnp.zeros((TP, LANES), F32)
    for i in range(STEPS):
        rows = slice(TP * i, TP * i + TP)
        gated = acc[0, rows, :] * jax.nn.sigmoid(acc[1, rows, :])
        gbuf[rows, :] = gated
        sums = jnp.where(lane == i, jnp.sum(gated * gated, axis=1, keepdims=True), sums)
    ss[...] = sums
    qcopies = []
    for k in FAR_FIRST:
        peer = lax.rem(me + k, TP)
        copy = pltpu.make_async_remote_copy(
            ss, sr.at[me], qs_sem.at[k - 1], qr_sem.at[k - 1], device_id={"tp": peer}, device_id_type=MESH
        )
        copy.start()
        qcopies.append(copy)
    sr[me] = ss[...]
    loads[9].wait()
    for k in range(1, TP):
        source = lax.rem(me + TP - k, TP)
        pltpu.make_async_remote_copy(
            ss, sr.at[source], qs_sem.at[k - 1], qr_sem.at[k - 1], device_id={"tp": source}, device_id_type=MESH
        ).wait_recv()
    squares = sr[0]
    for k in range(1, TP):
        squares = squares + sr[k]
    scale = lax.rsqrt(squares * (1.0 / D) + NORM_EPS)
    for i in range(STEPS):
        done = gbuf[i * TP : (i + 1) * TP, :] * scale[:, i : i + 1] * nout_v[...]
        for q in range(2):
            of[q, pl.ds(i, TP, stride=STEPS), :] = done[:, q * LANES : (q + 1) * LANES]
    for q in range(2):
        out[:, q * LANES : (q + 1) * LANES] = of[q].astype(BF16)

    for copy in xcopies + ycopies + qcopies:
        copy.wait_send()
    for k in range(1, reach + 1):

        @pl.when(me_z + k < nz)
        def _(k=k):
            zcopy(k, me_z + k).wait_send()

    for n in range(16):
        gcopy(n, me, 0, partner).wait_send()
    pcopy(0, me, 0, CHUNKS).wait_send()
    for n in range(1, 5):
        pcopy(n, me, 0, 2).wait_send()


def on_device(nz, ny, tokens, norm_in, decay_log, phase, b_real, b_imag, c_real, c_imag, skip_gain, w_value, w_gate, norm_out):
    def by_channel(b):
        return b.transpose(0, 2, 1).reshape(WIDTH, STATE)

    dma = pltpu.SemaphoreType.DMA
    scratch = [
        pltpu.VMEM((STEPS, D), BF16),
        pltpu.VMEM((1, D), F32),
        pltpu.VMEM((GROUPS, STATE), F32),
        pltpu.VMEM((GROUPS, STATE), F32),
        pltpu.VMEM((2, WIDTH, STATE), F32),
        pltpu.VMEM((2, WIDTH, STATE), F32),
        pltpu.VMEM((1, WIDTH), F32),
        pltpu.VMEM((D, WIDTH), BF16),
        pltpu.VMEM((D, WIDTH), BF16),
        pltpu.VMEM((1, WIDTH), F32),
        pltpu.VMEM((TP, STEPS, WIDTH), BF16),
        pltpu.VMEM((TP, STEPS, WIDTH), BF16),
        pltpu.VMEM((2, ROWS, LANES), F32),
        pltpu.VMEM((PAIRS, 2 * LANES, 2 * LANES), BF16),
        pltpu.VMEM((PAIRS, 2 * LANES, 2 * LANES), BF16),
        pltpu.VMEM((PAIRS, 2, ROWS, LANES), F32),
        pltpu.VMEM((2, GROUPS, STATE), F32),
        pltpu.VMEM((2, GROUPS, LANES), F32),
        pltpu.VMEM((2, PAIRS, LANES), F32),
        pltpu.VMEM((2, TP * PAIRS, LANES), F32),
        pltpu.VMEM((ny, 2, PAIRS, LANES), F32),
        pltpu.VMEM((PAIRS, 2, TP, LANES), F32),
        pltpu.VMEM((2, PAIRS, LANES), F32),
        pltpu.VMEM((ny, 2, PAIRS, LANES), F32),
        pltpu.VMEM((2, 2, PAIRS, LANES), F32),
        pltpu.VMEM((CHAIN, 2, PAIRS, LANES), F32),
        pltpu.VMEM((2, PAIRS, LANES), F32),
        pltpu.VMEM((PAIRS, ROWS, 2 * LANES), BF16),
        pltpu.VMEM((2, ROWS, LANES), F32),
        pltpu.VMEM((TP, ROWS, WIDTH), BF16),
        pltpu.VMEM((2, ROWS, WIDTH), F32),
        pltpu.VMEM((ROWS, WIDTH), F32),
        pltpu.VMEM((TP, LANES), F32),
        pltpu.VMEM((TP, TP, LANES), F32),
        pltpu.VMEM((2, ROWS, LANES), F32),
        dma((12,)),
        dma((TP - 1,)),
        dma((TP - 1,)),
        dma((max(ny - 1, 1),)),
        dma((max(ny - 1, 1),)),
        dma((CHAIN,)),
        dma((CHAIN,)),
        pltpu.SemaphoreType.REGULAR((CHAIN,)),
        dma((16,)),
        dma((16,)),
        dma((5,)),
        dma((5,)),
        dma((TP - 1,)),
        dma((TP - 1,)),
    ]
    operands = [
        pltpu.with_memory_space_constraint(operand, pltpu.HBM)
        for operand in (
            tokens,
            norm_in.reshape(1, D),
            decay_log,
            phase,
            by_channel(b_real),
            by_channel(b_imag),
            c_real.reshape(WIDTH, STATE),
            c_imag.reshape(WIDTH, STATE),
            skip_gain.reshape(1, WIDTH),
            w_value,
            w_gate,
            norm_out.reshape(1, WIDTH),
        )
    ]
    return pl.pallas_call(
        functools.partial(kernel, nz, ny),
        out_shape=jax.ShapeDtypeStruct((ROWS, WIDTH), BF16),
        in_specs=[pl.BlockSpec(memory_space=pltpu.HBM)] * 12,
        out_specs=pl.BlockSpec(memory_space=pltpu.VMEM),
        scratch_shapes=scratch,
        compiler_params=pltpu.CompilerParams(
            collective_id=0, has_side_effects=True, vmem_limit_bytes=48 * 1024 * 1024
        ),
        name="mixer",
    )(*operands)


def solution(mesh):
    torus = Mesh(mesh.devices.reshape(-1, 8, mesh.shape["tp"]), SP_TP)
    return on_torus(torus)


def on_torus(torus):
    in_specs = (
        P(SP_TP, None),
        P(),
        P("tp", None),
        P("tp", None),
        P("tp", None, None),
        P("tp", None, None),
        P("tp", None, None),
        P("tp", None, None),
        P("tp"),
        P(None, "tp"),
        P(None, "tp"),
        P("tp"),
    )
    return jax.shard_map(
        functools.partial(on_device, torus.shape["sp_0"], torus.shape["sp_1"]),
        mesh=torus,
        in_specs=in_specs,
        out_specs=P(SP, "tp"),
        check_vma=False,
    )
```

```python
import functools

import jax
import jax.numpy as jnp
from jax import lax
from jax.experimental import pallas as pl
from jax.experimental.pallas import tpu as pltpu
from jax.sharding import Mesh
from jax.sharding import PartitionSpec as P

D = 2048
SP = ("sp_0", "sp_1")
SP_TP = ("sp_0", "sp_1", "tp")
NORM_EPS = 1e-06

F32 = jnp.float32
BF16 = jnp.bfloat16
ROWS = 192
TP = 8
STEPS = 24
WIDTH = 256
GROUPS = 16
STATE = 64
PAIRS = 8
LANES = 128
CHAIN = 4
FAR_FIRST = (4, 3, 5, 2, 6, 1, 7)
CHUNKS = 4
ASKER, SCOUT = 1, 3
MESH = pl.DeviceIdType.MESH


def cmul(a, b):
    return (a[0] * b[0] - a[1] * b[1], a[0] * b[1] + a[1] * b[0])


def cmuladd(a, b, c):
    return (a[0] * b[0] - a[1] * b[1] + c[0], a[0] * b[1] + a[1] * b[0] + c[1])


def split_store(dst, g, real, imag):
    pair, second = g // 2, g % 2
    blank = jnp.zeros((16, STATE), F32)
    wide = [jnp.concatenate([blank, part] if second else [part, blank], axis=1) for part in (real, imag)]
    full = jnp.concatenate(wide, axis=1)
    high = full.astype(BF16)
    low = (full - high.astype(F32)).astype(BF16)
    row = 32 * (pair % 4) + 16 * second
    dst[pair, row : row + 16, :] = high
    dst[pair, LANES + row : LANES + row + 16, :] = low


def kernel(
    nz,
    ny,
    tok,
    nin,
    dl,
    ph,
    b_re,
    b_im,
    c_re,
    c_im,
    skip,
    wv,
    wg,
    nout,
    out,
    tok_v,
    nin_v,
    dl_v,
    ph_v,
    b_v,
    c_v,
    skip_v,
    wv_v,
    wg_v,
    nout_v,
    xs,
    xr,
    uf,
    wb,
    ct,
    dbuf,
    coef_v,
    wide_v,
    lam_v,
    pow_v,
    hop_v,
    fbuf,
    es,
    yr,
    zs,
    zr,
    held_v,
    sbuf,
    yv,
    zg,
    acc,
    gbuf,
    ss,
    sr,
    of,
    in_sem,
    xs_sem,
    xr_sem,
    ys_sem,
    yr_sem,
    zs_sem,
    zr_sem,
    here_sem,
    go_sem,
    asked_sem,
    gs_sem,
    gr_sem,
    ps_sem,
    pr_sem,
    qs_sem,
    qr_sem,
):
    me_z, me_y, me = lax.axis_index("sp_0"), lax.axis_index("sp_1"), lax.axis_index("tp")
    y_order = [k for k in FAR_FIRST if k < ny]
    reach = min(CHAIN, nz - 1)

    loads = [
        pltpu.make_async_copy(src, dst, in_sem.at[k])
        for k, (src, dst) in enumerate(
            (
                (tok, tok_v),
                (nin, nin_v),
                (dl, dl_v),
                (ph, ph_v),
                (b_re, b_v.at[0]),
                (b_im, b_v.at[1]),
                (c_re, c_v.at[0]),
                (c_im, c_v.at[1]),
                (skip, skip_v),
                (nout, nout_v),
                (wv, wv_v),
                (wg, wg_v),
            )
        )
    ]
    for load in loads[:2]:
        load.start()

    barrier = pltpu.get_barrier_semaphore()
    scout, asker = me == SCOUT, me == ASKER
    knows_y = (me != 0) & (me != SCOUT)

    def signal_tp(sem, peer):
        pl.semaphore_signal(sem, inc=1, device_id={"tp": peer}, device_id_type=MESH)

    def signal_y(sem, k):
        pl.semaphore_signal(sem, inc=1, device_id={"sp_1": lax.rem(me_y + k, ny)}, device_id_type=MESH)

    def signal_z(sem, k):
        pl.semaphore_signal(sem, inc=1, device_id={"sp_0": me_z + k}, device_id_type=MESH)

    for k in FAR_FIRST:
        signal_tp(barrier, lax.rem(me + k, TP))

    @pl.when(knows_y)
    def _():
        for k in y_order:
            signal_y(barrier, k)

    pl.when(scout & (me_z > 0))(lambda: signal_z(barrier, -1))
    pl.when(scout & (me_z + 1 < nz))(lambda: signal_z(barrier, 1))
    for load in loads[2:]:
        load.start()

    def tell_z(r):
        if r <= reach:
            pl.when(scout & (me_z > 0) & (me_z + r - 1 < nz))(lambda: signal_z(here_sem.at[r - 1], -1))

    def hear_z(r):
        if r <= reach:
            pl.when(scout & (me_z + r < nz))(lambda: pl.semaphore_wait(here_sem.at[r - 1], 1))

    loads[0].wait()
    loads[1].wait()
    x = tok_v[...].astype(F32)
    mean = jnp.sum(x * x, axis=1, keepdims=True) * (1.0 / D)
    normed = (x * lax.rsqrt(mean + NORM_EPS) * nin_v[...]).astype(BF16)
    for k in range(TP):
        xs[k] = normed[:, k * WIDTH : (k + 1) * WIDTH]

    neighbours = jnp.minimum(me_z, 1) + jnp.minimum(nz - 1 - me_z, 1)
    pl.semaphore_wait(barrier, TP - 1 + jnp.where(knows_y, ny - 1, 0) + jnp.where(scout, neighbours, 0))
    tell_z(1)

    @pl.when(asker)
    def _():
        for k in y_order:
            signal_y(asked_sem.at[0], k)

    xcopies = []
    for k in FAR_FIRST:
        peer = lax.rem(me + k, TP)
        copy = pltpu.make_async_remote_copy(
            xs.at[peer], xr.at[me], xs_sem.at[k - 1], xr_sem.at[k - 1], device_id={"tp": peer}, device_id_type=MESH
        )
        copy.start()
        xcopies.append(copy)
    xr[me] = xs[me]

    loads[2].wait()
    loads[3].wait()
    decay, phase = dl_v[...], ph_v[...]
    magnitude = jnp.exp(decay)
    bar_re, bar_im = magnitude * jnp.cos(phase), magnitude * jnp.sin(phase)
    modulus = decay * decay + phase * phase
    coef_v[0] = ((bar_re - 1.0) * decay + bar_im * phase) / modulus
    coef_v[1] = (bar_im * decay - (bar_re - 1.0) * phase) / modulus
    wide_v[0] = jnp.concatenate([bar_re, bar_re], axis=1)
    wide_v[1] = jnp.concatenate([bar_im, bar_im], axis=1)
    left_half = lax.broadcasted_iota(jnp.int32, (PAIRS, LANES), 1) < STATE
    lam = tuple(
        jnp.where(left_half, wide_v[k, pl.ds(0, PAIRS, stride=2), :], wide_v[k, pl.ds(1, PAIRS, stride=2), :])
        for k in range(2)
    )
    lam2 = cmul(lam, lam)
    lam4 = cmul(lam2, lam2)
    lam8 = cmul(lam4, lam4)
    seg = cmul(cmul(lam8, lam8), lam8)
    lam_v[0], lam_v[1] = lam
    power = (jnp.ones((PAIRS, LANES), F32), jnp.zeros((PAIRS, LANES), F32))
    for j in range(TP):
        pow_v[0, j * PAIRS : (j + 1) * PAIRS, :], pow_v[1, j * PAIRS : (j + 1) * PAIRS, :] = power
        power = cmul(power, seg)
    hop = power
    power = (jnp.ones((PAIRS, LANES), F32), jnp.zeros((PAIRS, LANES), F32))
    for y in range(ny):
        hop_v[y, 0], hop_v[y, 1] = power
        power = cmul(power, hop)
    line = power
    loads[4].wait()
    loads[5].wait()
    wb[...] = jnp.zeros_like(wb)
    for g in range(GROUPS):
        split_store(wb, g, b_v[0, 16 * g : 16 * g + 16, :], b_v[1, 16 * g : 16 * g + 16, :])

    for r in range(1, 3):
        hear_z(r)
        tell_z(r + 1)
    for k in range(1, TP):
        source = lax.rem(me + TP - k, TP)
        pltpu.make_async_remote_copy(
            xs.at[source], xr.at[source], xs_sem.at[k - 1], xr_sem.at[k - 1], device_id={"tp": source}, device_id_type=MESH
        ).wait_recv()

    for j in range(TP):
        block = xr[j].astype(F32)
        for q in range(2):
            uf[q, j * STEPS : (j + 1) * STEPS, :] = block[:, q * LANES : (q + 1) * LANES]
    for q in range(2):
        half = uf[q].astype(BF16)
        twice = jnp.concatenate([half, half], axis=1)
        for pair in range(4 * q, 4 * q + 4):
            drive = jnp.dot(twice, wb[pair], preferred_element_type=F32)
            dbuf[pair, 0] = drive[:, :LANES]
            dbuf[pair, 1] = drive[:, LANES:]

    def rate(pair):
        return tuple(jnp.broadcast_to(lam_v[k, pair : pair + 1, :], (TP, LANES)) for k in range(2))

    rates = [rate(pair) for pair in range(PAIRS)]

    def drive_at(pair, i):
        return (dbuf[pair, 0, pl.ds(i, TP, stride=STEPS), :], dbuf[pair, 1, pl.ds(i, TP, stride=STEPS), :])

    def first_pass(i, states):
        states = list(states)
        for sub in range(2):
            for pair in range(PAIRS):
                states[pair] = cmuladd(rates[pair], states[pair], drive_at(pair, 2 * i + sub))
        return tuple(states)

    nothing = jnp.zeros((TP, LANES), F32)
    ends = lax.fori_loop(0, STEPS // 2, first_pass, tuple((nothing, nothing) for _ in range(PAIRS)))
    segment = lax.broadcasted_iota(jnp.int32, (TP, LANES), 0)
    for pair in range(PAIRS):
        total = ends[pair]
        for shift in (1, 2, 4):
            moved = tuple(jnp.where(segment >= shift, pltpu.roll(part, shift, 0), 0.0) for part in total)
            decay_of = tuple(
                jnp.broadcast_to(pow_v[k, shift * PAIRS + pair : shift * PAIRS + pair + 1, :], (TP, LANES))
                for k in range(2)
            )
            total = cmuladd(decay_of, moved, total)
        for k in range(2):
            es[k, pair : pair + 1, :] = total[k][TP - 1 : TP, :]
            fbuf[pair, k] = jnp.where(segment >= 1, pltpu.roll(total[k], 1, 0), 0.0)

    pl.when(~knows_y)(lambda: pl.semaphore_wait(go_sem.at[0], 1))
    ycopies = []
    for k in y_order:
        peer = lax.rem(me_y + k, ny)
        copy = pltpu.make_async_remote_copy(
            es, yr.at[me_y], ys_sem.at[k - 1], yr_sem.at[k - 1], device_id={"sp_1": peer}, device_id_type=MESH
        )
        copy.start()
        ycopies.append(copy)
    yr[me_y] = es[...]

    @pl.when(asker)
    def _():
        if ny > 1:
            pl.semaphore_wait(asked_sem.at[0], ny - 1)
        signal_tp(go_sem.at[0], 0)
        signal_tp(go_sem.at[0], SCOUT)

    for r in range(3, reach + 1):
        hear_z(r)
        tell_z(r + 1)

    @pl.when(scout)
    def _():
        for k in FAR_FIRST:
            signal_tp(go_sem.at[1], (SCOUT + k) % TP)

    loads[6].wait()
    loads[7].wait()
    ct[...] = jnp.zeros_like(ct)
    for g in range(GROUPS):
        own = (c_v[0, 16 * g : 16 * g + 16, :], c_v[1, 16 * g : 16 * g + 16, :])
        real, imag = cmul(own, (coef_v[0, g : g + 1, :], coef_v[1, g : g + 1, :]))
        split_store(ct, g, real, -imag)

    for k in range(1, ny):
        source = lax.rem(me_y + ny - k, ny)
        pltpu.make_async_remote_copy(
            es, yr.at[source], ys_sem.at[k - 1], yr_sem.at[k - 1], device_id={"sp_1": source}, device_id_type=MESH
        ).wait_recv()
    empty = (jnp.zeros((PAIRS, LANES), F32), jnp.zeros((PAIRS, LANES), F32))
    total, inside = empty, empty
    for y in range(ny):
        inside = tuple(jnp.where(me_y == y, new, old) for new, old in zip(total, inside))
        total = cmuladd(hop, total, (yr[y, 0], yr[y, 1]))
    zs[0, 0], zs[0, 1] = total
    def zcopy(k, peer):
        return pltpu.make_async_remote_copy(
            zs.at[k // CHAIN],
            zr.at[k - 1],
            zs_sem.at[k - 1],
            zr_sem.at[k - 1],
            device_id={"sp_0": peer},
            device_id_type=MESH,
        )

    def zsend(k):
        @pl.when(me_z + k < nz)
        def _():
            zcopy(k, me_z + k).start()

    pl.when(me != SCOUT)(lambda: pl.semaphore_wait(go_sem.at[1], 1))
    for k in range(min(reach, CHAIN - 1), 0, -1):
        zsend(k)
    held_v[...] = jnp.zeros_like(held_v)
    for k in range(reach, 0, -1):

        @pl.when(me_z >= k)
        def _(k=k):
            zcopy(k, me_z - k).wait_recv()
            new = cmuladd(line, (held_v[0], held_v[1]), (zr[k - 1, 0], zr[k - 1, 1]))
            held_v[0], held_v[1] = new

    if reach == CHAIN:
        zs[1, 0], zs[1, 1] = cmuladd(line, (held_v[0], held_v[1]), total)
        zsend(CHAIN)
    held = cmuladd((hop_v[me_y, 0], hop_v[me_y, 1]), (held_v[0], held_v[1]), inside)
    held_v[0], held_v[1] = held

    starts = []
    for pair in range(PAIRS):
        carried = tuple(jnp.broadcast_to(held_v[k, pair : pair + 1, :], (TP, LANES)) for k in range(2))
        since = tuple(pow_v[k, pl.ds(pair, TP, stride=PAIRS), :] for k in range(2))
        starts.append(cmuladd(since, carried, (fbuf[pair, 0], fbuf[pair, 1])))

    def second_pass(i, states):
        states = list(states)
        row = pl.multiple_of(2 * TP * i, 2 * TP)
        for pair in range(PAIRS):
            one = cmuladd(rates[pair], states[pair], drive_at(pair, 2 * i))
            two = cmuladd(rates[pair], one, drive_at(pair, 2 * i + 1))
            for k in range(2):
                both = jnp.concatenate([one[k], two[k]], axis=0).astype(BF16)
                sbuf[pair, pl.ds(row, 2 * TP), k * LANES : (k + 1) * LANES] = both
            states[pair] = two
        return tuple(states)

    lax.fori_loop(0, STEPS // 2, second_pass, tuple(starts))

    loads[8].wait()
    for q in range(2):
        both = None
        for pair in range(4 * q, 4 * q + 4):
            part = lax.dot_general(sbuf[pair], ct[pair], (((1,), (1,)), ((), ())), preferred_element_type=F32)
            both = part if both is None else both + part
        yv[q] = both[:, :LANES] + both[:, LANES:]

    def activate(i, _):
        row = pl.multiple_of(2 * TP * i, 2 * TP)
        for q in range(2):
            gain = skip_v[:, q * LANES : (q + 1) * LANES]
            direct = jnp.concatenate([uf[q, pl.ds(2 * i + sub, TP, stride=STEPS), :] for sub in range(2)], axis=0)
            pre = yv[q, pl.ds(row, 2 * TP), :] + gain * direct
            z = jax.nn.gelu(pre)
            zg[me, pl.ds(row, 2 * TP), q * LANES : (q + 1) * LANES] = z.astype(BF16)
        return 0

    lax.fori_loop(0, STEPS // 2, activate, 0)

    chip, core = lax.div(me, 2), lax.rem(me, 2)
    partner = me + 1 - 2 * core
    right = lax.rem(chip + 1, TP // 2) * 2 + core
    left = lax.rem(chip + TP // 2 - 1, TP // 2) * 2 + core
    far = lax.rem(chip + 2, TP // 2) * 2 + core
    other = 1 - 2 * core

    def rows_of(owner, chunk, count):
        return zg.at[owner, pl.ds(chunk * (ROWS // CHUNKS), count * (ROWS // CHUNKS)), :]

    def gcopy(n, owner, chunk, peer):
        part = rows_of(owner, chunk, 1)
        return pltpu.make_async_remote_copy(
            part, part, gs_sem.at[n], gr_sem.at[n], device_id={"tp": peer}, device_id_type=MESH
        )

    def pcopy(n, owner, chunk, count):
        part = rows_of(owner, chunk, count)
        return pltpu.make_async_remote_copy(
            part, part, ps_sem.at[n], pr_sem.at[n], device_id={"tp": partner}, device_id_type=MESH
        )

    def project(owner, first=False):
        rows = pl.ds(pl.multiple_of(owner * WIDTH, WIDTH), WIDTH)
        block = zg[owner]
        for k, weight in enumerate((wv_v, wg_v)):
            part = jnp.dot(block, weight[rows, :], preferred_element_type=F32)
            if first:
                acc[k] = part
            else:
                acc[k] += part

    right_order, left_order = (0, 1, 2, 3), (2, 3, 0, 1)
    for k in range(CHUNKS):
        gcopy(right_order[k], me, right_order[k], right).start()
        gcopy(4 + left_order[k], me, left_order[k], left).start()
        if k == 0:
            pcopy(0, me, 0, CHUNKS).start()

    loads[10].wait()
    loads[11].wait()
    project(me, first=True)
    pcopy(0, partner, 0, CHUNKS).wait_recv()
    project(partner)
    for k in range(2):
        gcopy(k, left, k, left).wait_recv()
        gcopy(8 + k, left, k, right).start()
        gcopy(4 + 2 + k, right, 2 + k, right).wait_recv()
        gcopy(8 + 2 + k, right, 2 + k, left).start()
    pcopy(1, left, 0, 2).start()
    pcopy(2, right, 2, 2).start()
    for k in range(2):
        gcopy(2 + k, left, 2 + k, left).wait_recv()
        gcopy(4 + k, right, k, right).wait_recv()
    pcopy(3, left, 2, 2).start()
    pcopy(4, right, 0, 2).start()
    project(left)
    project(right)
    for k in range(2):
        gcopy(8 + k, far, k, left).wait_recv()
        gcopy(12 + k, far, k, partner).start()
        gcopy(8 + 2 + k, far, 2 + k, right).wait_recv()
        gcopy(12 + 2 + k, far, 2 + k, partner).start()
    pcopy(1, left + other, 0, 2).wait_recv()
    pcopy(3, left + other, 2, 2).wait_recv()
    project(left + other)
    pcopy(2, right + other, 2, 2).wait_recv()
    pcopy(4, right + other, 0, 2).wait_recv()
    project(right + other)
    project(far)
    for k in range(CHUNKS):
        gcopy(12 + k, far + other, k, partner).wait_recv()
    project(far + other)

    lane = lax.broadcasted_iota(jnp.int32, (TP, LANES), 1)
    sums = jnp.zeros((TP, LANES), F32)
    for i in range(STEPS):
        rows = slice(TP * i, TP * i + TP)
        gated = acc[0, rows, :] * jax.nn.sigmoid(acc[1, rows, :])
        gbuf[rows, :] = gated
        sums = jnp.where(lane == i, jnp.sum(gated * gated, axis=1, keepdims=True), sums)
    ss[...] = sums
    qcopies = []
    for k in FAR_FIRST:
        peer = lax.rem(me + k, TP)
        copy = pltpu.make_async_remote_copy(
            ss, sr.at[me], qs_sem.at[k - 1], qr_sem.at[k - 1], device_id={"tp": peer}, device_id_type=MESH
        )
        copy.start()
        qcopies.append(copy)
    sr[me] = ss[...]
    loads[9].wait()
    for k in range(1, TP):
        source = lax.rem(me + TP - k, TP)
        pltpu.make_async_remote_copy(
            ss, sr.at[source], qs_sem.at[k - 1], qr_sem.at[k - 1], device_id={"tp": source}, device_id_type=MESH
        ).wait_recv()
    squares = sr[0]
    for k in range(1, TP):
        squares = squares + sr[k]
    scale = lax.rsqrt(squares * (1.0 / D) + NORM_EPS)
    for i in range(STEPS):
        done = gbuf[i * TP : (i + 1) * TP, :] * scale[:, i : i + 1] * nout_v[...]
        for q in range(2):
            of[q, pl.ds(i, TP, stride=STEPS), :] = done[:, q * LANES : (q + 1) * LANES]
    for q in range(2):
        out[:, q * LANES : (q + 1) * LANES] = of[q].astype(BF16)

    for copy in xcopies + ycopies + qcopies:
        copy.wait_send()
    for k in range(1, reach + 1):

        @pl.when(me_z + k < nz)
        def _(k=k):
            zcopy(k, me_z + k).wait_send()

    for n in range(16):
        gcopy(n, me, 0, partner).wait_send()
    pcopy(0, me, 0, CHUNKS).wait_send()
    for n in range(1, 5):
        pcopy(n, me, 0, 2).wait_send()


def on_device(nz, ny, tokens, norm_in, decay_log, phase, b_real, b_imag, c_real, c_imag, skip_gain, w_value, w_gate, norm_out):
    def by_channel(b):
        return b.transpose(0, 2, 1).reshape(WIDTH, STATE)

    dma = pltpu.SemaphoreType.DMA
    scratch = [
        pltpu.VMEM((STEPS, D), BF16),
        pltpu.VMEM((1, D), F32),
        pltpu.VMEM((GROUPS, STATE), F32),
        pltpu.VMEM((GROUPS, STATE), F32),
        pltpu.VMEM((2, WIDTH, STATE), F32),
        pltpu.VMEM((2, WIDTH, STATE), F32),
        pltpu.VMEM((1, WIDTH), F32),
        pltpu.VMEM((D, WIDTH), BF16),
        pltpu.VMEM((D, WIDTH), BF16),
        pltpu.VMEM((1, WIDTH), F32),
        pltpu.VMEM((TP, STEPS, WIDTH), BF16),
        pltpu.VMEM((TP, STEPS, WIDTH), BF16),
        pltpu.VMEM((2, ROWS, LANES), F32),
        pltpu.VMEM((PAIRS, 2 * LANES, 2 * LANES), BF16),
        pltpu.VMEM((PAIRS, 2 * LANES, 2 * LANES), BF16),
        pltpu.VMEM((PAIRS, 2, ROWS, LANES), F32),
        pltpu.VMEM((2, GROUPS, STATE), F32),
        pltpu.VMEM((2, GROUPS, LANES), F32),
        pltpu.VMEM((2, PAIRS, LANES), F32),
        pltpu.VMEM((2, TP * PAIRS, LANES), F32),
        pltpu.VMEM((ny, 2, PAIRS, LANES), F32),
        pltpu.VMEM((PAIRS, 2, TP, LANES), F32),
        pltpu.VMEM((2, PAIRS, LANES), F32),
        pltpu.VMEM((ny, 2, PAIRS, LANES), F32),
        pltpu.VMEM((2, 2, PAIRS, LANES), F32),
        pltpu.VMEM((CHAIN, 2, PAIRS, LANES), F32),
        pltpu.VMEM((2, PAIRS, LANES), F32),
        pltpu.VMEM((PAIRS, ROWS, 2 * LANES), BF16),
        pltpu.VMEM((2, ROWS, LANES), F32),
        pltpu.VMEM((TP, ROWS, WIDTH), BF16),
        pltpu.VMEM((2, ROWS, WIDTH), F32),
        pltpu.VMEM((ROWS, WIDTH), F32),
        pltpu.VMEM((TP, LANES), F32),
        pltpu.VMEM((TP, TP, LANES), F32),
        pltpu.VMEM((2, ROWS, LANES), F32),
        dma((12,)),
        dma((TP - 1,)),
        dma((TP - 1,)),
        dma((max(ny - 1, 1),)),
        dma((max(ny - 1, 1),)),
        dma((CHAIN,)),
        dma((CHAIN,)),
        pltpu.SemaphoreType.REGULAR((CHAIN,)),
        pltpu.SemaphoreType.REGULAR((2,)),
        pltpu.SemaphoreType.REGULAR((1,)),
        dma((16,)),
        dma((16,)),
        dma((5,)),
        dma((5,)),
        dma((TP - 1,)),
        dma((TP - 1,)),
    ]
    operands = [
        pltpu.with_memory_space_constraint(operand, pltpu.HBM)
        for operand in (
            tokens,
            norm_in.reshape(1, D),
            decay_log,
            phase,
            by_channel(b_real),
            by_channel(b_imag),
            c_real.reshape(WIDTH, STATE),
            c_imag.reshape(WIDTH, STATE),
            skip_gain.reshape(1, WIDTH),
            w_value,
            w_gate,
            norm_out.reshape(1, WIDTH),
        )
    ]
    return pl.pallas_call(
        functools.partial(kernel, nz, ny),
        out_shape=jax.ShapeDtypeStruct((ROWS, WIDTH), BF16),
        in_specs=[pl.BlockSpec(memory_space=pltpu.HBM)] * 12,
        out_specs=pl.BlockSpec(memory_space=pltpu.VMEM),
        scratch_shapes=scratch,
        compiler_params=pltpu.CompilerParams(
            collective_id=0, has_side_effects=True, vmem_limit_bytes=48 * 1024 * 1024
        ),
        name="mixer",
    )(*operands)


def solution(mesh):
    torus = Mesh(mesh.devices.reshape(-1, 8, mesh.shape["tp"]), SP_TP)
    return on_torus(torus)


def on_torus(torus):
    in_specs = (
        P(SP_TP, None),
        P(),
        P("tp", None),
        P("tp", None),
        P("tp", None, None),
        P("tp", None, None),
        P("tp", None, None),
        P("tp", None, None),
        P("tp"),
        P(None, "tp"),
        P(None, "tp"),
        P("tp"),
    )
    return jax.shard_map(
        functools.partial(on_device, torus.shape["sp_0"], torus.shape["sp_1"]),
        mesh=torus,
        in_specs=in_specs,
        out_specs=P(SP, "tp"),
        check_vma=False,
    )
```
